256 devices in a mesh: grp: 4 (over y, x), ep: 64 (over z, core).
Axes of the slice: x: 2, y: 2, z: 32, core: 2. Of those that a mesh axis runs over, the one named last changes fastest.
The devices are a block of a 4x8x32 slice.
Arguments:
- tokens: bfloat16 [2048, 2048], P(('grp', 'ep')), parts along dimension 0, may hold values from -6 to 6
- first_gain: bfloat16 [2048], replicated, may hold values from 0.099609375 to 1.8984375
- query_weight: bfloat16 [2048, 1024], P(None, 'ep'), may hold values from -0.125 to 0.125
- key_weight: bfloat16 [2048, 1024], P(None, 'ep'), may hold values from -0.125 to 0.125
- value_weight: bfloat16 [2048, 1024], P(None, 'ep'), may hold values from -0.125 to 0.125
- outgate_weight: bfloat16 [2048, 1024], P(None, 'ep'), may hold values from -0.125 to 0.125
- igate_weight: bfloat16 [2048, 8], replicated, may hold values from -0.125 to 0.125
- fgate_weight: bfloat16 [2048, 8], replicated, may hold values from -0.125 to 0.125
- igate_bias: float32 [8], replicated, may hold values from -2 to 1
- fgate_bias: float32 [8], replicated, may hold values from -1 to 4
- memory_state: float32 [2048, 8, 128, 128], P(('grp', 'ep')), parts along dimension 0, may hold values from -0.6 to 0.6
- norm_state: float32 [2048, 8, 128], P(('grp', 'ep')), parts along dimension 0, may hold values from -0.6 to 0.6
- max_state: float32 [2048, 8], P(('grp', 'ep')), parts along dimension 0, may hold values from -1 to 2
- head_gain: bfloat16 [1024], replicated, may hold values from 0.099609375 to 1.8984375
- out_weight: bfloat16 [1024, 2048], P('ep'), may hold values from -0.1875 to 0.1875
- second_gain: bfloat16 [2048], replicated, may hold values from 0.099609375 to 1.8984375
- expert_ids: int32 [2048, 6], P(('grp', 'ep')), parts along dimension 0, may hold values from 0 to 63, all different within a row; in each aligned block of 8 rows (0 to 7, 8 to 15, ...) at most 2 rows name the same one
- route_weight: float32 [2048, 6], P(('grp', 'ep')), parts along dimension 0, may hold values from 0.2 to 1
- expert_gate: bfloat16 [64, 2048, 256], P('ep'), may hold values from -0.125 to 0.125
- expert_up: bfloat16 [64, 2048, 256], P('ep'), may hold values from -0.125 to 0.125
- expert_down: bfloat16 [64, 256, 2048], P('ep'), may hold values from -0.375 to 0.375
- shared_gate: bfloat16 [2048, 256], P('ep'), may hold values from -0.125 to 0.125
- shared_up: bfloat16 [2048, 256], P('ep'), may hold values from -0.125 to 0.125
- shared_down: bfloat16 [256, 2048], P(None, 'ep'), may hold values from -0.375 to 0.375
Outputs:
- mixed_out: bfloat16 [2048, 2048], P(('grp', 'ep')), parts along dimension 0
- memory_next: float32 [2048, 8, 128, 128], P(('grp', 'ep')), parts along dimension 0
- norm_next: float32 [2048, 8, 128], P(('grp', 'ep')), parts along dimension 0
- max_next: float32 [2048, 8], P(('grp', 'ep')), parts along dimension 0
The draws below stay inside these ranges and needn't reach their ends.
There are 4 independent parts, one for each index of `grp`. The reference program is written for one: setup_inputs(seed, part) draws one part's arguments, and reference() takes and returns one part's arrays. A program takes and returns all parts, laid end to end along the dimension named above; an argument that names none is the same for every part. Nothing has to cross between parts.
Inputs may be any that keep to these rules, and one draw needn't show every extreme that they name: `expert_ids`: each row names 6 different experts. Among the rows of one device no expert is named by more than 2 rows, and in every draw some expert is named by exactly 2 rows of some device.
All inputs are finite; a program needn't handle non-finite values.
Results may differ from the reference program's by a relative error of at most 0.013.
Values may be sent and summed in bfloat16 or wider, within the bound.
No kernel may reach another device: no remote copies, remote signals or barrier semaphores. Data moves between devices by JAX's collectives and lax.ppermute only.
A program may use at most 64 MiB of HBM per device.

```python
import math
import jax
import jax.numpy as jnp
import numpy as np
from jax import lax

D = 2048
HEADS = 8
DK = 128
FE = 256
FS = 256
TOP_K = 6
SEQ_DEV = 8
MW = 1024
SEQS = 512
EXPERTS = 64
CAP = 2
N_EP = 64


def levels(own_key, shape, pieces, low, high):
    loudness, own = 1.0, jax.random.fold_in(own_key, 6)
    for axis_at, parts in pieces:
        draws = jnp.exp(jax.random.uniform(jax.random.fold_in(own, axis_at), (parts,), jnp.float32, low / len(pieces), high / len(pieces)))
        loudness = loudness * jnp.repeat(draws, shape[axis_at] // parts).reshape([-1 if axis == axis_at else 1 for axis in range(len(shape))])
    return loudness


def routed_block(key, own, number, rows, number_of, top, reach, slope):
    sequence = jax.random.permutation(key, number_of)
    crowded, usual = portions_of(number_of, rows * top, reach, slope, True), portions_of(number_of, rows * top, reach, slope, False)
    places = jnp.arange(number_of)

    def named(tallies, turn):
        used = int((tallies > 0).sum())
        fixed = max(1, used // 4)
        shifted = fixed + (places - fixed + turn * (used - fixed)) % max(1, number_of - fixed)
        return jnp.zeros((number_of,), jnp.int32).at[sequence[jnp.where(places < fixed, places, shifted)]].set(jnp.asarray(tallies, jnp.int32))

    tallies = jnp.where(number % 4 == 0, named(crowded, number // 4), named(usual, number - number // 4 - 1))
    mixed = jax.random.permutation(jax.random.fold_in(own, 3), number_of)
    giver, sink = mixed[0:number_of // 2 * 2:2], mixed[1:number_of // 2 * 2:2]
    room = jnp.minimum(tallies[giver] - 1, reach - tallies[sink]) // 2
    room = jnp.where((giver == sequence[0]) | (sink == sequence[0]) | (tallies[sink] == 0), 0, jnp.maximum(room, 0))
    shifted = jax.random.randint(jax.random.fold_in(own, 4), (number_of // 2,), 0, 1 << 20) % (room + 1)
    tallies = tallies.at[giver].add(-shifted).at[sink].add(shifted)
    items = jnp.searchsorted(jnp.cumsum(tallies), jnp.arange(rows * top), side="right").astype(jnp.int32)
    listing = items.reshape(top, rows).T
    listing = listing[jax.random.permutation(jax.random.fold_in(own, 1), rows)]
    turn = jax.random.randint(jax.random.fold_in(own, 2), (rows, 1), 0, top)
    return jnp.take_along_axis(listing, (jnp.arange(top)[None, :] + turn) % top, axis=1)


def portions_of(number_of, total, limit, slope, full):
    portions = [(1 << 20) // math.isqrt(rank ** slope) + 1 for rank in range(1, number_of + 1)]
    largest = limit if full else min(limit, max(-(-total // number_of), total * portions[0] // sum(portions)))
    least = 1 if total - largest >= number_of - 1 else 0
    given, rest = [largest] + [least] * (number_of - 1), total - largest - least * (number_of - 1)
    while rest > 0:
        candidates = [i for i in range(1, number_of) if given[i] < largest] or [i for i in range(1, number_of) if given[i] < limit]
        mass, budget = sum([portions[i] for i in candidates]), rest
        for i in candidates:
            addition = min(limit - given[i], max(1, budget * portions[i] // mass), rest)
            given[i] = given[i] + addition
            rest = rest - addition
    return np.array(given)


def noise(key, shape, spread, limit, split=(), kind=jnp.bfloat16):
    loudness = levels(key, shape, split, -0.22, 0.18) if split else 1.0
    drawn = jax.random.normal(key, shape, jnp.float32) * spread * loudness
    return jnp.minimum(jnp.maximum(drawn, -limit), limit).astype(kind)


def setup_inputs(seed: int = 0, part: int = 0) -> dict:
    arg_keys = jax.random.split(jax.random.key(seed), 25)
    own_keys = jax.random.split(jax.random.fold_in(arg_keys[24], part), 25)
    tokens = noise(own_keys[0], (SEQS, D), 1.0, 6.0, ((0, 64),))
    first_gain = jnp.clip(1.0 + 0.18 * jax.random.normal(arg_keys[1], (D,), jnp.float32), 0.099609375, 1.8984375).astype(jnp.bfloat16)
    query_weight = noise(arg_keys[2], (D, MW), D ** -0.5, 0.125, ((1, 64),))
    key_weight = noise(arg_keys[3], (D, MW), D ** -0.5, 0.125, ((1, 64),))
    value_weight = noise(arg_keys[4], (D, MW), D ** -0.5, 0.125, ((1, 64),))
    outgate_weight = noise(arg_keys[5], (D, MW), D ** -0.5, 0.125, ((1, 64),))
    igate_weight = noise(arg_keys[6], (D, HEADS), D ** -0.5, 0.125)
    fgate_weight = noise(arg_keys[7], (D, HEADS), D ** -0.5, 0.125)
    igate_bias = jnp.clip(jax.random.uniform(arg_keys[8], (HEADS,), jnp.float32, -2.0, 1.0), -2.0, 1.0)
    fgate_bias = jnp.clip(jax.random.uniform(arg_keys[9], (HEADS,), jnp.float32, -1.0, 4.0), -1.0, 4.0)
    memory_state = noise(own_keys[10], (SEQS, HEADS, DK, DK), 0.1, 0.6, ((0, 64),), jnp.float32)
    norm_state = noise(own_keys[11], (SEQS, HEADS, DK), 0.1, 0.6, ((0, 64),), jnp.float32)
    max_state = jnp.clip(-1.0 + 3.0 * jax.random.uniform(own_keys[12], (SEQS, HEADS), jnp.float32) ** levels(own_keys[12], (SEQS, HEADS), ((0, 64),), -0.2, 0.2), -1.0, 2.0)
    head_gain = jnp.clip(1.0 + 0.18 * jax.random.normal(arg_keys[13], (MW,), jnp.float32), 0.099609375, 1.8984375).astype(jnp.bfloat16)
    out_weight = noise(arg_keys[14], (MW, D), MW ** -0.5, 0.1875, ((0, 64),))
    second_gain = jnp.clip(1.0 + 0.18 * jax.random.normal(arg_keys[15], (D,), jnp.float32), 0.099609375, 1.8984375).astype(jnp.bfloat16)
    expert_ids_keys = jax.random.split(jax.random.fold_in(own_keys[16], 1), SEQS // SEQ_DEV)
    expert_ids_turns = jax.random.permutation(jax.random.fold_in(own_keys[16], 3), SEQS // SEQ_DEV)
    expert_ids = jax.vmap(lambda own, number: routed_block(jax.random.fold_in(own_keys[16], 2), own, number, SEQ_DEV, EXPERTS, TOP_K, CAP, 1))(expert_ids_keys, expert_ids_turns).reshape((SEQS, TOP_K))
    route_weight = jnp.clip(0.2 + 0.8 * jax.random.uniform(own_keys[17], (SEQS, TOP_K), jnp.float32) ** levels(own_keys[17], (SEQS, TOP_K), ((0, 64),), -0.2, 0.2), 0.2, 1.0)
    expert_gate = noise(arg_keys[18], (EXPERTS, D, FE), D ** -0.5, 0.125, ((0, 64),))
    expert_up = noise(arg_keys[19], (EXPERTS, D, FE), D ** -0.5, 0.125, ((0, 64),))
    expert_down = noise(arg_keys[20], (EXPERTS, FE, D), FE ** -0.5, 0.375, ((0, 64),))
    shared_gate = noise(arg_keys[21], (D, FS), D ** -0.5, 0.125, ((0, 64),))
    shared_up = noise(arg_keys[22], (D, FS), D ** -0.5, 0.125, ((0, 64),))
    shared_down = noise(arg_keys[23], (FS, D), FS ** -0.5, 0.375, ((1, 64),))
    return dict(tokens=tokens, first_gain=first_gain, query_weight=query_weight, key_weight=key_weight, value_weight=value_weight, outgate_weight=outgate_weight, igate_weight=igate_weight, fgate_weight=fgate_weight, igate_bias=igate_bias, fgate_bias=fgate_bias, memory_state=memory_state, norm_state=norm_state, max_state=max_state, head_gain=head_gain, out_weight=out_weight, second_gain=second_gain, expert_ids=expert_ids, route_weight=route_weight, expert_gate=expert_gate, expert_up=expert_up, expert_down=expert_down, shared_gate=shared_gate, shared_up=shared_up, shared_down=shared_down)


epsilon = 1e-06

def rms_scale(values, gain):
    return values * lax.rsqrt(lax.optimization_barrier(jnp.mean(values * values, axis=-1, keepdims=True)) + epsilon) * gain.astype(jnp.float32)

def cell_step(normed, query, key_proj, value_proj, outgate, igate_weight, fgate_weight, igate_bias, fgate_bias, memory_state, norm_state, max_state, head_gain):
    row_count, head_count = max_state.shape
    head_size = memory_state.shape[-1]
    input_gate = jnp.dot(normed, igate_weight, preferred_element_type=jnp.float32) + igate_bias
    forget_log = jax.nn.log_sigmoid(jnp.dot(normed, fgate_weight, preferred_element_type=jnp.float32) + fgate_bias)
    query_heads = query.astype(jnp.float32).reshape(row_count, head_count, head_size)
    key_heads = key_proj.astype(jnp.float32).reshape(row_count, head_count, head_size) * head_size ** (-0.5)
    value_heads = value_proj.astype(jnp.float32).reshape(row_count, head_count, head_size)
    max_next = jnp.maximum(forget_log + max_state, input_gate)
    decay_rate = jnp.exp(forget_log + max_state - max_next)
    injected = jnp.exp(input_gate - max_next)
    memory_next = decay_rate[:, :, None, None] * memory_state + injected[:, :, None, None] * (key_heads[:, :, :, None] * value_heads[:, :, None, :])
    norm_next = decay_rate[:, :, None] * norm_state + injected[:, :, None] * key_heads
    numerator = jnp.einsum('shd,shde->she', query_heads, memory_next, precision=lax.Precision.HIGHEST)
    denominator = jnp.maximum(jnp.abs(lax.optimization_barrier(jnp.sum(query_heads * norm_next, axis=-1))), jnp.exp(-max_next))
    readout = numerator / denominator[:, :, None]
    readout = rms_scale(readout, head_gain.reshape(head_count, head_size))
    gated = readout.reshape(row_count, head_count * head_size) * jax.nn.sigmoid(outgate.astype(jnp.float32))
    return (gated.astype(jnp.bfloat16), memory_next, norm_next, max_next)

def expert_apply(picked_rows, gate_matrix, up_matrix, down_matrix):
    gate_sums = jnp.dot(picked_rows, gate_matrix, preferred_element_type=jnp.float32)
    up_sums = jnp.dot(picked_rows, up_matrix, preferred_element_type=jnp.float32)
    hidden = (jax.nn.silu(gate_sums) * up_sums).astype(jnp.bfloat16)
    return jnp.dot(hidden, down_matrix, preferred_element_type=jnp.float32).astype(jnp.bfloat16)

def reference(tokens, first_gain, query_weight, key_weight, value_weight, outgate_weight, igate_weight, fgate_weight, igate_bias, fgate_bias, memory_state, norm_state, max_state, head_gain, out_weight, second_gain, expert_ids, route_weight, expert_gate, expert_up, expert_down, shared_gate, shared_up, shared_down):
    inputs = tokens.astype(jnp.float32)
    normed = rms_scale(inputs, first_gain).astype(jnp.bfloat16)
    query = jnp.dot(normed, query_weight, preferred_element_type=jnp.float32).astype(jnp.bfloat16)
    key_proj = jnp.dot(normed, key_weight, preferred_element_type=jnp.float32).astype(jnp.bfloat16)
    value_proj = jnp.dot(normed, value_weight, preferred_element_type=jnp.float32).astype(jnp.bfloat16)
    outgate = jnp.dot(normed, outgate_weight, preferred_element_type=jnp.float32).astype(jnp.bfloat16)
    gated, memory_next, norm_next, max_next = cell_step(normed, query, key_proj, value_proj, outgate, igate_weight, fgate_weight, igate_bias, fgate_bias, memory_state, norm_state, max_state, head_gain)
    mix = jnp.dot(gated, out_weight, preferred_element_type=jnp.float32).astype(jnp.bfloat16)
    stream = inputs + mix.astype(jnp.float32)
    normed_two = rms_scale(stream, second_gain).astype(jnp.bfloat16)
    padded = jnp.concatenate([normed_two, jnp.zeros((1, D), normed_two.dtype)], axis=0)

    def per_expert(routed, inputs_expert):
        expert_index, gate_matrix, up_matrix, down_matrix = inputs_expert
        chosen = expert_ids == expert_index
        weight = lax.optimization_barrier(jnp.sum(jnp.where(chosen, route_weight, jnp.zeros_like(route_weight)), axis=1))
        weight_pad = jnp.concatenate([weight, jnp.zeros((1,), weight.dtype)], axis=0)
        picked = jnp.nonzero(jnp.any(chosen, axis=1), size=N_EP * CAP, fill_value=SEQS)[0].astype(jnp.int32)
        result = expert_apply(padded[picked], gate_matrix, up_matrix, down_matrix)
        routed = routed.at[picked].add(weight_pad[picked][:, None] * result.astype(routed.dtype), mode='drop')
        return (routed, None)
    routed, _ = lax.scan(per_expert, jnp.zeros((SEQS, D), jnp.float32), (jnp.arange(EXPERTS, dtype=jnp.int32), expert_gate, expert_up, expert_down))
    gate_shared = jnp.dot(normed_two, shared_gate, preferred_element_type=jnp.float32)
    up_shared = jnp.dot(normed_two, shared_up, preferred_element_type=jnp.float32)
    hidden_shared = (jax.nn.silu(gate_shared) * up_shared).astype(jnp.bfloat16)
    shared_result = jnp.dot(hidden_shared, shared_down, preferred_element_type=jnp.float32)
    mixed_out = (stream + routed + shared_result).astype(jnp.bfloat16)
    return (mixed_out, memory_next, norm_next, max_next)
```

```python
import jax
import jax.numpy as jnp
from jax import lax
from jax.sharding import Mesh
from jax.sharding import PartitionSpec as P

FAR = "za"
NEAR = ("zb", "core")
RING = ("za", "zb")
EP = ("za", "zb", "core")
GRP_EP = ("grp", "za", "zb", "core")

epsilon = 1e-06


def rms_scale(values, gain):
    return (
        values
        * lax.rsqrt(jnp.mean(values * values, axis=-1, keepdims=True) + epsilon)
        * gain.astype(jnp.float32)
    )


def cell_step(
    normed,
    query,
    key_proj,
    value_proj,
    outgate,
    igate_weight,
    fgate_weight,
    igate_bias,
    fgate_bias,
    memory_state,
    norm_state,
    max_state,
    head_gain,
):
    row_count, head_count = max_state.shape
    head_size = memory_state.shape[-1]
    input_gate = jnp.dot(normed, igate_weight, preferred_element_type=jnp.float32) + igate_bias
    forget_log = jax.nn.log_sigmoid(
        jnp.dot(normed, fgate_weight, preferred_element_type=jnp.float32) + fgate_bias
    )
    query_heads = query.astype(jnp.float32).reshape(row_count, head_count, head_size)
    key_heads = key_proj.astype(jnp.float32).reshape(
        row_count, head_count, head_size
    ) * head_size ** (-0.5)
    value_heads = value_proj.astype(jnp.float32).reshape(row_count, head_count, head_size)
    max_next = jnp.maximum(forget_log + max_state, input_gate)
    decay_rate = jnp.exp(forget_log + max_state - max_next)
    injected = jnp.exp(input_gate - max_next)
    memory_next = decay_rate[:, :, None, None] * memory_state + injected[:, :, None, None] * (
        key_heads[:, :, :, None] * value_heads[:, :, None, :]
    )
    norm_next = decay_rate[:, :, None] * norm_state + injected[:, :, None] * key_heads
    numerator = jnp.einsum(
        "shd,shde->she", query_heads, memory_next, precision=lax.Precision.HIGHEST
    )
    denominator = jnp.maximum(
        jnp.abs(jnp.sum(query_heads * norm_next, axis=-1)), jnp.exp(-max_next)
    )
    readout = numerator / denominator[:, :, None]
    readout = rms_scale(readout, head_gain.reshape(head_count, head_size))
    gated = readout.reshape(row_count, head_count * head_size) * jax.nn.sigmoid(
        outgate.astype(jnp.float32)
    )
    return (gated.astype(jnp.bfloat16), memory_next, norm_next, max_next)


def rounded(values, kind):
    info = jnp.finfo(kind)
    return lax.reduce_precision(values, info.nexp, info.nmant)


def earlier_count(named, axis):
    count = named.shape[axis]
    before = jnp.arange(count)[:, None] < jnp.arange(count)[None, :]
    moved = jnp.moveaxis(named, axis, -1)
    counts = jnp.sum(jnp.where(before, moved[..., :, None], 0.0), axis=-2)
    return jnp.moveaxis(counts, -1, axis)


def split_two(values, kind):
    high = rounded(values, kind)
    return high.astype(kind), (values - high).astype(kind)


def shards(
    tokens,
    first_gain,
    query_weight,
    key_weight,
    value_weight,
    outgate_weight,
    igate_weight,
    fgate_weight,
    igate_bias,
    fgate_bias,
    memory_state,
    norm_state,
    max_state,
    head_gain,
    out_weight,
    second_gain,
    expert_ids,
    route_weight,
    expert_gate,
    expert_up,
    expert_down,
    shared_gate,
    shared_up,
    shared_down,
):
    f32, bf16, f16 = jnp.float32, jnp.bfloat16, jnp.float16
    rows, width = tokens.shape
    top = expert_ids.shape[1]
    far = lax.axis_size(FAR)
    near_z = lax.axis_size("zb")
    cores = lax.axis_size("core")
    near = near_z * cores
    ring = far * near_z
    devices = ring * cores
    slots = max(2, 2 * rows * top // devices)
    my_far = lax.axis_index(FAR)
    my_zb = lax.axis_index("zb")
    my_core = lax.axis_index("core")
    swap = [(i, (i + 1) % cores) for i in range(cores)]

    half = width // 2
    hidden = shared_gate.shape[1]
    packed = jnp.concatenate(
        [
            jnp.concatenate([out_weight[:, :half], out_weight[:, half:]], axis=0),
            shared_gate,
            shared_up,
            shared_down.T,
        ],
        axis=1,
    )
    whole = lax.all_gather(packed, EP, axis=0, tiled=True)

    own = jnp.concatenate([query_weight.T, key_weight.T, value_weight.T, outgate_weight.T], axis=0)
    other = lax.ppermute(own, "core", swap)

    inputs = tokens.astype(f32)
    normed_exact = rounded(rms_scale(inputs, first_gain), bf16)
    normed = normed_exact.astype(bf16)
    weight_high, weight_low = split_two(route_weight, f16)
    notes = jnp.concatenate([expert_ids.astype(f16), weight_high, weight_low], axis=1)
    notes = jnp.pad(notes, ((0, 0), (0, 128 - notes.shape[1])))
    gathered = lax.all_gather(
        jnp.concatenate([normed_exact.astype(f16), notes], axis=1), RING, axis=0, tiled=True
    )
    block_rows = gathered[:, :width].astype(bf16)
    my_notes = gathered[:, width:]
    other_notes = lax.ppermute(my_notes, "core", swap)

    pair = jnp.where(my_core == 0, jnp.stack([own, other]), jnp.stack([other, own]))
    columns = lax.dot_general(
        block_rows, pair.reshape(-1, width), (((1,), (1,)), ((), ())), preferred_element_type=f32
    ).astype(bf16)
    projected = lax.all_to_all(
        columns.reshape(ring, rows, columns.shape[1]), RING, split_axis=0, concat_axis=0, tiled=True
    )
    share = query_weight.shape[1]
    projected = projected.reshape(ring, rows, cores, 4, share).transpose(3, 1, 0, 2, 4)
    projected = projected.reshape(4, rows, devices * share)

    mine = my_notes.reshape(far, near_z, rows, 128)
    theirs = other_notes.reshape(far, near_z, rows, 128)
    both = jnp.where(my_core == 0, jnp.stack([mine, theirs], 2), jnp.stack([theirs, mine], 2))
    me = (my_far * near + my_zb * cores + my_core).astype(f32)
    named = jnp.any(both[..., :top].astype(f32) == me, axis=-1).astype(f32)
    place = earlier_count(named, 3)
    slot_ids = jnp.arange(slots, dtype=f32)
    picks = named[..., None] * (place[..., None] == slot_ids)
    picks = picks.transpose(1, 2, 0, 4, 3).reshape(near, far, slots, rows)
    source = jnp.arange(far)[None, :, None, None] * near + jnp.arange(near)[:, None, None, None]
    selector = jnp.where(
        source[..., None] == jnp.arange(devices)[:, None], picks[:, :, :, None, :], 0.0
    )
    selector = selector.reshape(near * far * slots, devices * rows).astype(bf16)
    at_mine = lax.dynamic_index_in_dim(mine, my_zb, axis=1, keepdims=False).astype(f32)
    block_experts = (my_far * near).astype(f32) + jnp.arange(near, dtype=f32)
    hits = (at_mine[:, :, :top, None] == block_experts).astype(f32)
    weights = at_mine[:, :, top : 2 * top] + at_mine[:, :, 2 * top : 3 * top]
    hit = jnp.sum(hits, axis=2)
    hit_weight = jnp.sum(hits * weights[..., None], axis=2)
    hit_place = earlier_count(hit, 1)
    mixer = hit_weight[..., None] * (hit_place[..., None] == slot_ids) * hit[..., None]
    mixer = jnp.where(
        (jnp.arange(far)[:, None] == jnp.arange(far))[:, None, None, :, None],
        mixer[:, :, :, None, :],
        0.0,
    )
    mixer = mixer.reshape(far * rows, near * far * slots)
    mixer_high, mixer_low = split_two(mixer, bf16)

    gated, memory_next, norm_next, max_next = cell_step(
        normed,
        projected[0],
        projected[1],
        projected[2],
        projected[3],
        igate_weight,
        fgate_weight,
        igate_bias,
        fgate_bias,
        memory_state,
        norm_state,
        max_state,
        head_gain,
    )
    spread = gated.reshape(1, rows, devices, 1, -1) * jnp.eye(2, dtype=bf16).reshape(2, 1, 1, 2, 1)
    mix_sums = jnp.dot(
        spread.reshape(2 * rows, -1), whole[:, :half], preferred_element_type=f32
    )
    mix_sums = jnp.concatenate([mix_sums[:rows], mix_sums[rows:]], axis=1)
    stream = inputs + mix_sums.astype(bf16).astype(f32)
    normed_exact = rounded(rms_scale(stream, second_gain), bf16)
    normed_two = normed_exact.astype(bf16)

    all_rows = lax.all_gather(normed_exact.astype(f16), EP, axis=0, tiled=True).astype(bf16)
    flat_rows = jnp.dot(selector, all_rows, preferred_element_type=f32).astype(bf16)
    gate_sums = jnp.dot(flat_rows, expert_gate[0], preferred_element_type=f32)
    up_sums = jnp.dot(flat_rows, expert_up[0], preferred_element_type=f32)
    hidden_rows = (jax.nn.silu(gate_sums) * up_sums).astype(bf16)
    result = jnp.dot(hidden_rows, expert_down[0], preferred_element_type=f32).astype(bf16)
    near_results = lax.all_to_all(
        result.reshape(near, far * slots, width), NEAR, split_axis=0, concat_axis=0, tiled=True
    ).reshape(near * far * slots, width)
    partial = jnp.dot(mixer_high, near_results, preferred_element_type=f32) + jnp.dot(
        mixer_low, near_results, preferred_element_type=f32
    )
    far_sums = lax.all_to_all(
        partial.astype(bf16).reshape(far, rows, width), FAR, split_axis=0, concat_axis=0, tiled=True
    )
    routed = jnp.sum(far_sums.astype(f32), axis=0)

    gate_up = jnp.dot(normed_two, whole[:, half : half + 2 * hidden], preferred_element_type=f32)
    hidden_shared = (jax.nn.silu(gate_up[:, :hidden]) * gate_up[:, hidden:]).astype(bf16)
    shared_result = lax.dot_general(
        hidden_shared,
        whole[:, half + 2 * hidden :],
        (((1,), (1,)), ((), ())),
        preferred_element_type=f32,
    )
    mixed_out = (stream + routed + shared_result).astype(bf16)
    return (mixed_out, memory_next, norm_next, max_next)


def solution(mesh):
    torus = Mesh(
        mesh.devices.reshape(mesh.shape["grp"], 8, 4, 2), ("grp", "za", "zb", "core")
    )
    placed = (
        P(GRP_EP, None),
        P(),
        P(None, EP),
        P(None, EP),
        P(None, EP),
        P(None, EP),
        P(),
        P(),
        P(),
        P(),
        P(GRP_EP, None, None, None),
        P(GRP_EP, None, None),
        P(GRP_EP, None),
        P(),
        P(EP, None),
        P(),
        P(GRP_EP, None),
        P(GRP_EP, None),
        P(EP, None, None),
        P(EP, None, None),
        P(EP, None, None),
        P(EP, None),
        P(EP, None),
        P(None, EP),
    )
    return jax.shard_map(
        shards,
        mesh=torus,
        in_specs=placed,
        out_specs=(
            P(GRP_EP, None),
            P(GRP_EP, None, None, None),
            P(GRP_EP, None, None),
            P(GRP_EP, None),
        ),
        check_vma=False,
    )
```

```python
import jax
import jax.numpy as jnp
from jax import lax
from jax.sharding import Mesh
from jax.sharding import PartitionSpec as P

FAR = "za"
NEAR = ("zb", "core")
RING = ("za", "zb")
EP = ("za", "zb", "core")
GRP_EP = ("grp", "za", "zb", "core")

epsilon = 1e-06


def rms_scale(values, gain):
    return (
        values
        * lax.rsqrt(jnp.mean(values * values, axis=-1, keepdims=True) + epsilon)
        * gain.astype(jnp.float32)
    )


def cell_step(
    normed,
    query,
    key_proj,
    value_proj,
    outgate,
    igate_weight,
    fgate_weight,
    igate_bias,
    fgate_bias,
    memory_state,
    norm_state,
    max_state,
    head_gain,
):
    row_count, head_count = max_state.shape
    head_size = memory_state.shape[-1]
    input_gate = jnp.dot(normed, igate_weight, preferred_element_type=jnp.float32) + igate_bias
    forget_log = jax.nn.log_sigmoid(
        jnp.dot(normed, fgate_weight, preferred_element_type=jnp.float32) + fgate_bias
    )
    query_heads = query.astype(jnp.float32).reshape(row_count, head_count, head_size)
    key_heads = key_proj.astype(jnp.float32).reshape(
        row_count, head_count, head_size
    ) * head_size ** (-0.5)
    value_heads = value_proj.astype(jnp.float32).reshape(row_count, head_count, head_size)
    max_next = jnp.maximum(forget_log + max_state, input_gate)
    decay_rate = jnp.exp(forget_log + max_state - max_next)
    injected = jnp.exp(input_gate - max_next)
    memory_next = decay_rate[:, :, None, None] * memory_state + injected[:, :, None, None] * (
        key_heads[:, :, :, None] * value_heads[:, :, None, :]
    )
    norm_next = decay_rate[:, :, None] * norm_state + injected[:, :, None] * key_heads
    numerator = jnp.einsum(
        "shd,shde->she", query_heads, memory_next, precision=lax.Precision.HIGHEST
    )
    denominator = jnp.maximum(
        jnp.abs(jnp.sum(query_heads * norm_next, axis=-1)), jnp.exp(-max_next)
    )
    readout = numerator / denominator[:, :, None]
    readout = rms_scale(readout, head_gain.reshape(head_count, head_size))
    gated = readout.reshape(row_count, head_count * head_size) * jax.nn.sigmoid(
        outgate.astype(jnp.float32)
    )
    return (gated.astype(jnp.bfloat16), memory_next, norm_next, max_next)


def rounded(values, kind):
    info = jnp.finfo(kind)
    return lax.reduce_precision(values, info.nexp, info.nmant)


def earlier_count(named, axis):
    count = named.shape[axis]
    before = jnp.arange(count)[:, None] < jnp.arange(count)[None, :]
    moved = jnp.moveaxis(named, axis, -1)
    counts = jnp.sum(jnp.where(before, moved[..., :, None], 0.0), axis=-2)
    return jnp.moveaxis(counts, -1, axis)


def split_two(values, kind):
    high = rounded(values, kind)
    return high.astype(kind), (values - high).astype(kind)


def shards(
    tokens,
    first_gain,
    query_weight,
    key_weight,
    value_weight,
    outgate_weight,
    igate_weight,
    fgate_weight,
    igate_bias,
    fgate_bias,
    memory_state,
    norm_state,
    max_state,
    head_gain,
    out_weight,
    second_gain,
    expert_ids,
    route_weight,
    expert_gate,
    expert_up,
    expert_down,
    shared_gate,
    shared_up,
    shared_down,
):
    f32, bf16, f16 = jnp.float32, jnp.bfloat16, jnp.float16
    rows, width = tokens.shape
    top = expert_ids.shape[1]
    far = lax.axis_size(FAR)
    near_z = lax.axis_size("zb")
    cores = lax.axis_size("core")
    near = near_z * cores
    ring = far * near_z
    devices = ring * cores
    slots = max(2, 2 * rows * top // devices)
    my_far = lax.axis_index(FAR)
    my_zb = lax.axis_index("zb")
    my_core = lax.axis_index("core")
    swap = [(i, (i + 1) % cores) for i in range(cores)]

    own = jnp.concatenate([query_weight.T, key_weight.T, value_weight.T, outgate_weight.T], axis=0)
    other = lax.ppermute(own, "core", swap)

    inputs = tokens.astype(f32)
    normed_exact = rounded(rms_scale(inputs, first_gain), bf16)
    normed = normed_exact.astype(bf16)
    weight_high, weight_low = split_two(route_weight, f16)
    notes = jnp.concatenate([expert_ids.astype(f16), weight_high, weight_low], axis=1)
    half = width // 2
    hidden = shared_gate.shape[1]
    cut = shared_gate.shape[0] // rows
    piece = width // cut
    notes = jnp.pad(notes, ((0, (cut - 1) * rows), (0, 128 - notes.shape[1])))
    payload = jnp.concatenate(
        [
            jnp.concatenate(
                [normed_exact[:, i * piece : (i + 1) * piece] for i in range(cut)], axis=0
            ).astype(f16),
            jnp.concatenate([out_weight[:, :half], out_weight[:, half:]], axis=0).astype(f16),
            shared_gate.astype(f16),
            shared_up.astype(f16),
            shared_down.T.astype(f16),
            notes,
        ],
        axis=1,
    )
    gathered = lax.all_gather(payload, EP, axis=0, tiled=True)
    whole = gathered[:, piece : piece + half + 3 * hidden]
    chips_rows = gathered[:, :piece].reshape(ring, cores, cut, rows, piece)
    chips_rows = lax.dynamic_index_in_dim(chips_rows, my_core, axis=1, keepdims=False)
    block_rows = chips_rows.transpose(0, 2, 1, 3).reshape(ring * rows, width).astype(bf16)
    my_notes = gathered[:, piece + half + 3 * hidden :].reshape(far, near, cut * rows, 128)
    my_notes = lax.dynamic_index_in_dim(
        my_notes[:, :, :rows], my_zb * cores + my_core, axis=1, keepdims=False
    ).astype(f32)

    pair = jnp.where(my_core == 0, jnp.stack([own, other]), jnp.stack([other, own]))
    columns = lax.dot_general(
        block_rows, pair.reshape(-1, width), (((1,), (1,)), ((), ())), preferred_element_type=f32
    ).astype(bf16)
    projected = lax.all_to_all(
        columns.reshape(ring, rows, columns.shape[1]), RING, split_axis=0, concat_axis=0, tiled=True
    )
    share = query_weight.shape[1]
    projected = projected.reshape(ring, rows, cores, 4, share).transpose(3, 1, 0, 2, 4)
    projected = projected.reshape(4, rows, devices * share)

    slot_ids = jnp.arange(slots, dtype=f32)
    at_mine = my_notes
    block_experts = (my_far * near).astype(f32) + jnp.arange(near, dtype=f32)
    hits = (at_mine[:, :, :top, None] == block_experts).astype(f32)
    weights = at_mine[:, :, top : 2 * top] + at_mine[:, :, 2 * top : 3 * top]
    hit = jnp.sum(hits, axis=2)
    hit_weight = jnp.sum(hits * weights[..., None], axis=2)
    hit_place = earlier_count(hit, 1)
    chosen = (hit_place[..., None] == slot_ids) * hit[..., None]
    same = (jnp.arange(far)[:, None] == jnp.arange(far))[:, None, None, :, None]
    chosen = jnp.where(same, chosen[:, :, :, None, :], 0.0)
    chosen = chosen.reshape(far * rows, near, far * slots)
    mixer = (chosen * hit_weight.reshape(far * rows, near, 1)).reshape(far * rows, -1)
    mixer_high, mixer_low = split_two(mixer, bf16)
    selector = chosen.reshape(far * rows, -1).astype(bf16)

    gated, memory_next, norm_next, max_next = cell_step(
        normed,
        projected[0],
        projected[1],
        projected[2],
        projected[3],
        igate_weight,
        fgate_weight,
        igate_bias,
        fgate_bias,
        memory_state,
        norm_state,
        max_state,
        head_gain,
    )
    spread = gated.reshape(1, rows, devices, 1, -1) * jnp.eye(2, dtype=bf16).reshape(2, 1, 1, 2, 1)
    mix_sums = jnp.dot(
        spread.reshape(2 * rows, -1), whole[:, :half].astype(bf16), preferred_element_type=f32
    )
    mix_sums = jnp.concatenate([mix_sums[:rows], mix_sums[rows:]], axis=1)
    stream = inputs + mix_sums.astype(bf16).astype(f32)
    normed_two = rounded(rms_scale(stream, second_gain), bf16).astype(bf16)

    far_rows = lax.all_gather(normed_two, FAR, axis=0, tiled=True)
    outgoing = lax.dot_general(
        selector, far_rows, (((0,), (0,)), ((), ())), preferred_element_type=f32
    ).astype(bf16)
    flat_rows = lax.all_to_all(
        outgoing.reshape(near, far * slots, width), NEAR, split_axis=0, concat_axis=0, tiled=True
    ).reshape(near * far * slots, width)
    gate_sums = jnp.dot(flat_rows, expert_gate[0], preferred_element_type=f32)
    up_sums = jnp.dot(flat_rows, expert_up[0], preferred_element_type=f32)
    hidden_rows = (jax.nn.silu(gate_sums) * up_sums).astype(bf16)
    result = jnp.dot(hidden_rows, expert_down[0], preferred_element_type=f32).astype(bf16)
    near_results = lax.all_to_all(
        result.reshape(near, far * slots, width), NEAR, split_axis=0, concat_axis=0, tiled=True
    ).reshape(near * far * slots, width)
    partial = jnp.dot(mixer_high, near_results, preferred_element_type=f32) + jnp.dot(
        mixer_low, near_results, preferred_element_type=f32
    )
    far_sums = lax.all_to_all(
        partial.astype(bf16).reshape(far, rows, width), FAR, split_axis=0, concat_axis=0, tiled=True
    )
    routed = jnp.sum(far_sums.astype(f32), axis=0)

    gate_up = jnp.dot(
        normed_two, whole[:, half : half + 2 * hidden].astype(bf16), preferred_element_type=f32
    )
    hidden_shared = (jax.nn.silu(gate_up[:, :hidden]) * gate_up[:, hidden:]).astype(bf16)
    shared_result = lax.dot_general(
        hidden_shared,
        whole[:, half + 2 * hidden :].astype(bf16),
        (((1,), (1,)), ((), ())),
        preferred_element_type=f32,
    )
    mixed_out = (stream + routed + shared_result).astype(bf16)
    return (mixed_out, memory_next, norm_next, max_next)


def solution(mesh):
    torus = Mesh(
        mesh.devices.reshape(mesh.shape["grp"], 8, 4, 2), ("grp", "za", "zb", "core")
    )
    placed = (
        P(GRP_EP, None),
        P(),
        P(None, EP),
        P(None, EP),
        P(None, EP),
        P(None, EP),
        P(),
        P(),
        P(),
        P(),
        P(GRP_EP, None, None, None),
        P(GRP_EP, None, None),
        P(GRP_EP, None),
        P(),
        P(EP, None),
        P(),
        P(GRP_EP, None),
        P(GRP_EP, None),
        P(EP, None, None),
        P(EP, None, None),
        P(EP, None, None),
        P(EP, None),
        P(EP, None),
        P(None, EP),
    )
    return jax.shard_map(
        shards,
        mesh=torus,
        in_specs=placed,
        out_specs=(
            P(GRP_EP, None),
            P(GRP_EP, None, None, None),
            P(GRP_EP, None, None),
            P(GRP_EP, None),
        ),
        check_vma=False,
    )
```

```python
import jax
import jax.numpy as jnp
from jax import lax
from jax.sharding import Mesh
from jax.sharding import PartitionSpec as P

FAR = "za"
NEAR = ("zm", "zb", "core")
ROW = ("za", "zm")
EP = ("za", "zm", "zb", "core")
GRP_EP = ("grp", "za", "zm", "zb", "core")

epsilon = 1e-06


def rms_scale(values, gain):
    return (
        values
        * lax.rsqrt(jnp.mean(values * values, axis=-1, keepdims=True) + epsilon)
        * gain.astype(jnp.float32)
    )


def cell_step(
    normed,
    query,
    key_proj,
    value_proj,
    outgate,
    igate_weight,
    fgate_weight,
    igate_bias,
    fgate_bias,
    memory_state,
    norm_state,
    max_state,
    head_gain,
):
    row_count, head_count = max_state.shape
    head_size = memory_state.shape[-1]
    input_gate = jnp.dot(normed, igate_weight, preferred_element_type=jnp.float32) + igate_bias
    forget_log = jax.nn.log_sigmoid(
        jnp.dot(normed, fgate_weight, preferred_element_type=jnp.float32) + fgate_bias
    )
    query_heads = query.astype(jnp.float32).reshape(row_count, head_count, head_size)
    key_heads = key_proj.astype(jnp.float32).reshape(
        row_count, head_count, head_size
    ) * head_size ** (-0.5)
    value_heads = value_proj.astype(jnp.float32).reshape(row_count, head_count, head_size)
    max_next = jnp.maximum(forget_log + max_state, input_gate)
    decay_rate = jnp.exp(forget_log + max_state - max_next)
    injected = jnp.exp(input_gate - max_next)
    memory_next = decay_rate[:, :, None, None] * memory_state + injected[:, :, None, None] * (
        key_heads[:, :, :, None] * value_heads[:, :, None, :]
    )
    norm_next = decay_rate[:, :, None] * norm_state + injected[:, :, None] * key_heads
    numerator = jnp.einsum(
        "shd,shde->she", query_heads, memory_next, precision=lax.Precision.HIGHEST
    )
    denominator = jnp.maximum(
        jnp.abs(jnp.sum(query_heads * norm_next, axis=-1)), jnp.exp(-max_next)
    )
    readout = numerator / denominator[:, :, None]
    readout = rms_scale(readout, head_gain.reshape(head_count, head_size))
    gated = readout.reshape(row_count, head_count * head_size) * jax.nn.sigmoid(
        outgate.astype(jnp.float32)
    )
    return (gated.astype(jnp.bfloat16), memory_next, norm_next, max_next)


def rounded(values, kind):
    info = jnp.finfo(kind)
    return lax.reduce_precision(values, info.nexp, info.nmant)


def from_peer(values, axis):
    return lax.ppermute(values, axis, [(0, 1), (1, 0)])


def in_order(values, axis_names, first):
    for place, name in enumerate(axis_names, first):
        values = jnp.where(lax.axis_index(name) == 0, values, jnp.flip(values, place))
    return values


def earlier_count(named, axis):
    count = named.shape[axis]
    before = jnp.arange(count)[:, None] < jnp.arange(count)[None, :]
    moved = jnp.moveaxis(named, axis, -1)
    counts = jnp.sum(jnp.where(before, moved[..., :, None], 0.0), axis=-2)
    return jnp.moveaxis(counts, -1, axis)


def split_two(values, kind):
    high = rounded(values, kind)
    return high.astype(kind), (values - high).astype(kind)


def shards(
    tokens,
    first_gain,
    query_weight,
    key_weight,
    value_weight,
    outgate_weight,
    igate_weight,
    fgate_weight,
    igate_bias,
    fgate_bias,
    memory_state,
    norm_state,
    max_state,
    head_gain,
    out_weight,
    second_gain,
    expert_ids,
    route_weight,
    expert_gate,
    expert_up,
    expert_down,
    shared_gate,
    shared_up,
    shared_down,
):
    f32, bf16, f16 = jnp.float32, jnp.bfloat16, jnp.float16
    rows, width = tokens.shape
    top = expert_ids.shape[1]
    far = lax.axis_size(FAR)
    near = lax.axis_size(NEAR)
    row = lax.axis_size(ROW)
    devices = far * near
    members = devices // row
    slots = max(2, 2 * rows * top // devices)
    my_far = lax.axis_index(FAR)
    share = query_weight.shape[1]

    own = jnp.concatenate([query_weight.T, key_weight.T, value_weight.T, outgate_weight.T], axis=0)
    beside = from_peer(own, "zb")

    inputs = tokens.astype(f32)
    normed_exact = rounded(rms_scale(inputs, first_gain), bf16)
    normed = normed_exact.astype(bf16)
    weight_high, weight_low = split_two(route_weight, f16)
    notes = jnp.concatenate([expert_ids.astype(f16), weight_high, weight_low], axis=1)
    notes = jnp.pad(notes, ((0, 0), (0, 128 - notes.shape[1])))
    out_parts = out_weight.shape[0] // rows
    payload = jnp.concatenate(
        [normed_exact.astype(f16)]
        + [out_weight[i * rows : (i + 1) * rows].astype(f16) for i in range(out_parts)]
        + [notes],
        axis=1,
    )
    payload, beside = lax.optimization_barrier((payload, beside))
    column_weights = jnp.concatenate([own, beside], axis=0)
    other_weights = from_peer(column_weights, "core")
    gathered = lax.all_gather(payload, ROW, axis=0, tiled=True)
    block_rows = gathered[:, :width].astype(bf16)
    out_own = gathered[:, width : width * (1 + out_parts)]
    out_beside = from_peer(out_own, "zb")
    my_notes = gathered[:, width * (1 + out_parts) :].reshape(far, row // far, rows, 128)
    at_mine = lax.dynamic_index_in_dim(
        my_notes, lax.axis_index("zm"), axis=1, keepdims=False
    ).astype(f32)

    columns = jnp.concatenate(
        [
            lax.dot_general(
                block_rows, weights, (((1,), (1,)), ((), ())), preferred_element_type=f32
            )
            for weights in (column_weights, other_weights)
        ],
        axis=1,
    ).astype(bf16)
    projected = lax.all_to_all(
        columns.reshape(row, rows, columns.shape[1]), ROW, split_axis=0, concat_axis=0, tiled=True
    )
    projected, out_beside = lax.optimization_barrier((projected, out_beside))
    out_pair = jnp.stack([out_own, out_beside])
    out_other = from_peer(out_pair, "core")
    projected = projected.reshape(row, rows, 2, 2, 4, share).transpose(4, 1, 0, 3, 2, 5)
    projected = in_order(projected, ("zb", "core"), 3)
    projected = projected.reshape(4, rows, devices * share)

    slot_ids = jnp.arange(slots, dtype=f32)
    block_experts = (my_far * near).astype(f32) + jnp.arange(near, dtype=f32)
    hits = (at_mine[:, :, :top, None] == block_experts).astype(f32)
    weights = at_mine[:, :, top : 2 * top] + at_mine[:, :, 2 * top : 3 * top]
    hit = jnp.sum(hits, axis=2)
    hit_weight = jnp.sum(hits * weights[..., None], axis=2)
    hit_place = earlier_count(hit, 1)
    chosen = (hit_place[..., None] == slot_ids) * hit[..., None]
    same = (jnp.arange(far)[:, None] == jnp.arange(far))[:, None, None, :, None]
    chosen = jnp.where(same, chosen[:, :, :, None, :], 0.0)
    chosen = chosen.reshape(far * rows, near, far * slots)
    mixer = (chosen * hit_weight.reshape(far * rows, near, 1)).reshape(far * rows, -1)
    mixer_high, mixer_low = split_two(mixer, bf16)
    selector = chosen.reshape(far * rows, -1).astype(bf16)

    gated, memory_next, norm_next, max_next = cell_step(
        normed,
        projected[0],
        projected[1],
        projected[2],
        projected[3],
        igate_weight,
        fgate_weight,
        igate_bias,
        fgate_bias,
        memory_state,
        norm_state,
        max_state,
        head_gain,
    )
    spread = gated.reshape(rows, row, 2, 2, out_parts, -1).transpose(3, 2, 4, 0, 1, 5)
    spread = in_order(spread, ("core", "zb"), 0).reshape(2, 2, out_parts, rows, -1)
    mix_sums = jnp.zeros((rows, width), f32)
    for core, halves in enumerate((out_pair, out_other)):
        for zb in range(2):
            for part in range(out_parts):
                mix_sums = mix_sums + jnp.dot(
                    spread[core, zb, part],
                    halves[zb, :, part * width : (part + 1) * width].astype(bf16),
                    preferred_element_type=f32,
                )
    stream = inputs + mix_sums.astype(bf16).astype(f32)
    normed_exact = rounded(rms_scale(stream, second_gain), bf16)
    normed_two = normed_exact.astype(bf16)

    hidden = shared_gate.shape[1]
    depth = shared_gate.shape[0]
    cut = depth // rows
    piece = width // cut
    payload = jnp.concatenate(
        [
            jnp.concatenate(
                [normed_exact[:, i * piece : (i + 1) * piece] for i in range(cut)], axis=0
            ).astype(f16),
            shared_gate.astype(f16),
            shared_up.astype(f16),
            shared_down.T.astype(f16),
        ],
        axis=1,
    )
    gathered = lax.all_gather(payload, FAR, axis=0, tiled=True)
    far_rows = gathered[:, :piece].reshape(far, cut, rows, piece).transpose(0, 2, 1, 3)
    far_rows = far_rows.reshape(far * rows, width).astype(bf16)
    shared_one = gathered[:, piece:]
    shared_beside = from_peer(shared_one, "zm")
    outgoing = lax.dot_general(
        selector, far_rows, (((0,), (0,)), ((), ())), preferred_element_type=f32
    ).astype(bf16)
    flat_rows = lax.all_to_all(
        outgoing.reshape(near, far * slots, width), NEAR, split_axis=0, concat_axis=0, tiled=True
    ).reshape(near * far * slots, width)
    flat_rows, shared_beside = lax.optimization_barrier((flat_rows, shared_beside))
    shared_two = jnp.stack([shared_one, shared_beside])
    shared_beside = from_peer(shared_two, "zb")
    gate_sums = jnp.dot(flat_rows, expert_gate[0], preferred_element_type=f32)
    up_sums = jnp.dot(flat_rows, expert_up[0], preferred_element_type=f32)
    hidden_rows = (jax.nn.silu(gate_sums) * up_sums).astype(bf16)
    result = jnp.dot(hidden_rows, expert_down[0], preferred_element_type=f32).astype(bf16)
    near_results = lax.all_to_all(
        result.reshape(near, far * slots, width), NEAR, split_axis=0, concat_axis=0, tiled=True
    ).reshape(near * far * slots, width)
    near_results, shared_beside = lax.optimization_barrier((near_results, shared_beside))
    shared_four = jnp.stack([shared_two, shared_beside])
    shared_other = from_peer(shared_four, "core")
    partial = jnp.dot(mixer_high, near_results, preferred_element_type=f32) + jnp.dot(
        mixer_low, near_results, preferred_element_type=f32
    )
    far_sums = lax.all_to_all(
        partial.astype(bf16).reshape(far, rows, width), FAR, split_axis=0, concat_axis=0, tiled=True
    )
    routed = jnp.sum(far_sums.astype(f32), axis=0)

    by_member = normed_two.reshape(rows, far, 2, 2, 2, depth).transpose(4, 3, 2, 0, 1, 5)
    by_member = in_order(by_member, ("core", "zb", "zm"), 0).reshape(near, rows, far * depth)
    shared_all = jnp.concatenate(
        [shared_four.reshape(near // 2, far * depth, -1), shared_other.reshape(near // 2, far * depth, -1)]
    ).astype(bf16)
    gate_up = lax.dot_general(
        by_member,
        shared_all[:, :, : 2 * hidden],
        (((2,), (1,)), ((0,), (0,))),
        preferred_element_type=f32,
    )
    gate_up = jnp.sum(gate_up, axis=0)
    hidden_shared = (jax.nn.silu(gate_up[:, :hidden]) * gate_up[:, hidden:]).astype(bf16)
    shared_result = lax.dot_general(
        hidden_shared,
        shared_all[:, :, 2 * hidden :],
        (((1,), (2,)), ((), ())),
        preferred_element_type=f32,
    )
    shared_result = shared_result.reshape(rows, 2, 2, 2, far, depth).transpose(0, 4, 3, 2, 1, 5)
    shared_result = in_order(shared_result, NEAR, 2).reshape(rows, width)
    mixed_out = (stream + routed + shared_result).astype(bf16)
    return (mixed_out, memory_next, norm_next, max_next)


def solution(mesh):
    torus = Mesh(
        mesh.devices.reshape(mesh.shape["grp"], 8, 2, 2, 2), GRP_EP
    )
    placed = (
        P(GRP_EP, None),
        P(),
        P(None, EP),
        P(None, EP),
        P(None, EP),
        P(None, EP),
        P(),
        P(),
        P(),
        P(),
        P(GRP_EP, None, None, None),
        P(GRP_EP, None, None),
        P(GRP_EP, None),
        P(),
        P(EP, None),
        P(),
        P(GRP_EP, None),
        P(GRP_EP, None),
        P(EP, None, None),
        P(EP, None, None),
        P(EP, None, None),
        P(EP, None),
        P(EP, None),
        P(None, EP),
    )
    return jax.shard_map(
        shards,
        mesh=torus,
        in_specs=placed,
        out_specs=(
            P(GRP_EP, None),
            P(GRP_EP, None, None, None),
            P(GRP_EP, None, None),
            P(GRP_EP, None),
        ),
        check_vma=False,
    )
```
